32 devices in a mesh: sp: 8 (over z, core), tp: 4 (over y, x).
Axes of the slice: x: 2, y: 2, z: 4, core: 2. Of those that a mesh axis runs over, the one named last changes fastest.
Arguments:
- tokens: bfloat16 [2048, 4096], P('sp'), may hold values from -6 to 6
- norm_gain: float32 [2, 4096], replicated, may hold values from 0.1 to 1.9
- w_outer: bfloat16 [2, 4096, 1024], P(None, 'sp', 'tp'), may hold values from -0.09375 to 0.09375
- w_inner: bfloat16 [2, 4096, 1024], P(None, 'sp', 'tp'), may hold values from -0.09375 to 0.09375
- w_value: bfloat16 [2, 4096, 1024], P(None, 'sp', 'tp'), may hold values from -0.09375 to 0.09375
- w_back: bfloat16 [2, 1024, 4096], P(None, 'sp', 'tp'), may hold values from -0.1875 to 0.1875
- taps: float32 [2, 3, 1024], P(None, None, 'tp'), may hold values from -3 to 3
Outputs:
- result: bfloat16 [2048, 4096], P('sp', 'tp')
The draws below stay inside these ranges and needn't reach their ends.
All inputs are finite; a program needn't handle non-finite values.
Results may differ from the reference program's by a relative error of at most 0.022.
Values may be sent and summed in bfloat16 or wider, within the bound.
A program may use at most 64 MiB of HBM per device.

```python
import jax
import jax.numpy as jnp
from jax import lax

D = 4096
MIX = 1024
LAYERS = 2
TAPS = 3
TOKENS = 2048


def level_of(own_key, shape, cuts, low, top_value):
    factor_of = 1.0
    for dim, blocks in cuts:
        draws = jax.random.uniform(jax.random.fold_in(jax.random.fold_in(own_key, 6), dim), (blocks,), jnp.float32, low / len(cuts), top_value / len(cuts))
        factor_of = factor_of * jnp.repeat(jnp.exp(draws), shape[dim] // blocks).reshape((-1,) + (1,) * (len(shape) - 1 - dim))
    return factor_of


def bell_draw(key, extent, spread, bound, split=(), dtype=jnp.bfloat16):
    loudness = level_of(key, extent, split, -0.22, 0.18) if split else 1.0
    result = jax.random.normal(key, extent, jnp.float32) * spread * loudness
    return jnp.minimum(jnp.maximum(result, -bound), bound).astype(dtype)


def setup_inputs(seed: int = 0) -> dict:
    key_list = jax.random.split(jax.random.key(seed), 8)
    return {
        "tokens": bell_draw(key_list[0], (TOKENS, D), 1.0, 6.0, ((0, 8),)),
        "norm_gain": jnp.clip(1.0 + 0.18 * jax.random.normal(key_list[1], (LAYERS, D), jnp.float32), 0.1, 1.9),
        "w_outer": bell_draw(key_list[2], (LAYERS, D, MIX), D ** -0.5, 0.09375, ((1, 8), (2, 4))),
        "w_inner": bell_draw(key_list[3], (LAYERS, D, MIX), D ** -0.5, 0.09375, ((1, 8), (2, 4))),
        "w_value": bell_draw(key_list[4], (LAYERS, D, MIX), D ** -0.5, 0.09375, ((1, 8), (2, 4))),
        "w_back": bell_draw(key_list[5], (LAYERS, MIX, D), MIX ** -0.5, 0.1875, ((1, 8), (2, 4))),
        "taps": bell_draw(key_list[6], (LAYERS, TAPS, MIX), 0.6, 3.0, ((2, 4),), jnp.float32),
    }


eps = 1e-06

def reference(tokens, norm_gain, w_outer, w_inner, w_value, w_back, taps):
    current = tokens
    for layer in range(LAYERS):
        xf = current.astype(jnp.float32)
        normed = (xf * lax.rsqrt(lax.optimization_barrier(jnp.mean(xf * xf, axis=-1, keepdims=True)) + eps) * norm_gain[layer]).astype(jnp.bfloat16)
        outer = jnp.dot(normed, w_outer[layer], preferred_element_type=jnp.float32).astype(jnp.bfloat16)
        inner = jnp.dot(normed, w_inner[layer], preferred_element_type=jnp.float32).astype(jnp.bfloat16)
        value = jnp.dot(normed, w_value[layer], preferred_element_type=jnp.float32).astype(jnp.bfloat16)
        mixed = (inner.astype(jnp.float32) * value.astype(jnp.float32)).astype(jnp.bfloat16)
        padded = jnp.pad(mixed.astype(jnp.float32), ((2, 0), (0, 0)))
        conv = taps[layer, 0] * padded[:-2] + taps[layer, 1] * padded[1:-1] + taps[layer, 2] * padded[2:]
        gated = (outer.astype(jnp.float32) * conv).astype(jnp.bfloat16)
        proj = jnp.dot(gated, w_back[layer], preferred_element_type=jnp.float32)
        current = (current.astype(jnp.float32) + proj).astype(jnp.bfloat16)
    return current
```

```python
import functools

import jax
import jax.numpy as jnp
from jax import lax
from jax.experimental import pallas as pl
from jax.experimental.pallas import tpu as pltpu
from jax.sharding import PartitionSpec as P

MESH = pl.DeviceIdType.MESH
f32 = jnp.float32
bf16 = jnp.bfloat16

eps = 1e-06


def shifted(block, axis, distance):
    devices = range(lax.axis_size(axis))
    route = [(i - distance, i) for i in devices if i - distance in devices]
    return lax.ppermute(block, axis, route)


def per_device(tokens, norm_gain, w_outer, w_inner, w_value, w_back, taps):
    layers = w_outer.shape[0]
    count = tokens.shape[0]
    feats = w_back.shape[2]
    own = lax.axis_index("tp")
    held = (
        lax.all_gather(w_outer, "sp", axis=1, tiled=True),
        lax.all_gather(w_inner, "sp", axis=1, tiled=True),
        lax.all_gather(w_value, "sp", axis=1, tiled=True),
        lax.all_gather(w_back, "sp", axis=1, tiled=True),
    )
    current = tokens
    resid = lax.dynamic_slice_in_dim(tokens, own * feats, feats, 1)
    for layer in range(layers):
        if layer > 0:
            current = lax.all_gather(resid, "tp", axis=1, tiled=True)
        xf = current.astype(jnp.float32)
        normed = (
            xf * lax.rsqrt(jnp.mean(xf * xf, axis=-1, keepdims=True) + eps) * norm_gain[layer]
        ).astype(jnp.bfloat16)
        outer = jnp.dot(normed, held[0][layer], preferred_element_type=jnp.float32)
        inner = jnp.dot(normed, held[1][layer], preferred_element_type=jnp.float32)
        value = jnp.dot(normed, held[2][layer], preferred_element_type=jnp.float32)
        outer = outer.astype(jnp.bfloat16)
        inner = inner.astype(jnp.bfloat16)
        value = value.astype(jnp.bfloat16)
        mixed = (inner.astype(jnp.float32) * value.astype(jnp.float32)).astype(jnp.bfloat16)
        before = shifted(mixed[count - 2 :], "sp", 1)
        padded = jnp.concatenate([before, mixed], axis=0).astype(jnp.float32)
        conv = (
            taps[layer, 0] * padded[:count]
            + taps[layer, 1] * padded[1 : count + 1]
            + taps[layer, 2] * padded[2:]
        )
        gated = (outer.astype(jnp.float32) * conv).astype(jnp.bfloat16)
        whole = lax.all_gather(gated, "tp", axis=1, tiled=True)
        proj = jnp.dot(whole, held[3][layer], preferred_element_type=jnp.float32)
        resid = (resid.astype(jnp.float32) + proj).astype(jnp.bfloat16)
    return resid


def mixer_kernel(
    tok, gain, w_outer, w_inner, w_value, w_back, taps, out,
    xs, win, wback, acc, ss, gat, mixed, halo, res, landed,
    sem_local, sem_tok_local, tok_send, tok_recv, w_send, w_recv,
    g_send, g_recv, h_send, h_recv, o_send, o_recv,
):
    s, t = lax.axis_index("sp"), lax.axis_index("tp")
    n_sp, n_tp = win.shape[1], xs.shape[1]
    layers = wback.shape[0]
    rows = tok.shape[0]
    feats = xs.shape[3]
    units = 4 * layers
    core = lax.rem(s, 2)
    flip = 1 - 2 * core
    left = s < n_sp // 2
    side = jnp.where(left, 1, -1)
    plane = lax.div(s, 2)
    is_end = jnp.logical_or(plane == 0, plane == n_sp // 2 - 1)
    is_mid = jnp.logical_not(is_end)
    partner = s + flip
    inward = jnp.where(is_end, s + 2 * side, s)
    end = jnp.where(is_mid, s - 2 * side, s)
    opp = jnp.where(is_mid, s + 2 * side, s)
    oppend = jnp.where(is_mid, s + 4 * side, s)
    tx = t + 1 - 2 * lax.rem(t, 2)
    ty = t + 2 - 4 * lax.div(t, 2)
    td = n_tp - 1 - t

    barrier = pltpu.get_barrier_semaphore()
    for k in range(1, n_sp):
        pl.semaphore_signal(barrier, inc=1, device_id=(lax.rem(s + k, n_sp), t), device_id_type=MESH)
    for other in (tx, ty):
        pl.semaphore_signal(barrier, inc=1, device_id=(s, other), device_id_type=MESH)
    pl.semaphore_wait(barrier, n_sp + 1)

    projections = (w_outer, w_inner, w_value)

    def own_w(u):
        layer, m = u // 4, u % 4
        return projections[m].at[layer] if m < 3 else w_back.at[layer]

    def held_w(u, source):
        layer, m = u // 4, u % 4
        return win.at[3 * layer + m, source] if m < 3 else wback.at[layer, source]

    def remote(a, b, ssem, rsem, sp, tp):
        return pltpu.make_async_remote_copy(
            src_ref=a, dst_ref=b, send_sem=ssem, recv_sem=rsem, device_id=(sp, tp), device_id_type=MESH
        )

    def send_w(u, source, kind, target, own=False):
        a = own_w(u) if own else held_w(u, source)
        remote(a, held_w(u, source), w_send.at[u, kind], w_recv.at[u, source], target, t).start()

    def wait_w(u, source):
        remote(held_w(u, source), held_w(u, source), w_send.at[u, 0], w_recv.at[u, source], partner, t).wait_recv()

    def tok_cols(j):
        return tok.at[:, pl.ds(pl.multiple_of(j * feats, feats), feats)]

    def tok_to_end_mid():
        target = lax.div(s, 2) + 2
        place = xs.at[0, t, pl.ds(pl.multiple_of(core * rows, rows), rows)]
        return remote(tok_cols(t), place, tok_send.at[0], tok_recv.at[core], target, t)

    outer_mid = jnp.logical_or(s == 2, s == n_sp - 3)
    my_half = pl.multiple_of(jnp.where(left, 1, 0) * rows, rows)
    partner_half = pl.multiple_of(jnp.where(left, 0, 1) * rows, rows)

    def tok_local(j):
        return pltpu.make_async_copy(tok_cols(j), xs.at[0, j, pl.ds(my_half, rows)], sem_tok_local.at[j])

    def tok_partner(j):
        return remote(tok_cols(j), xs.at[0, j, pl.ds(partner_half, rows)], tok_send.at[j], tok_recv.at[j], partner, t)

    def result_copy(b):
        return remote(res.at[b], landed, o_send.at[b], o_recv, 2 * (s - 2) + b, t)

    def result_wait():
        remote(landed, landed, o_send.at[0], o_recv, partner, t).wait_recv()
        out[...] = landed[...]

    @pl.when(is_end)
    def _():
        sends = []
        for u in range(units):
            send_w(u, s, 0, inward, own=True)
            if u == 0:
                tok_to_end_mid().start()
        for u in range(units):
            remote(own_w(u), held_w(u, s), w_send.at[u, 0], w_recv.at[u, s], inward, t).wait_send()
        tok_to_end_mid().wait_send()
        result_wait()

    def gather_pieces(g, buf):
        size = buf.shape[1] // 2
        def piece(block, half, k, target):
            ref = buf.at[block, pl.ds(half * size, size)]
            return remote(ref, ref, g_send.at[g, k], g_recv.at[g, k], s, target)
        return piece

    def gather_start(g, buf):
        p = gather_pieces(g, buf)
        p(t, 0, 0, tx).start()
        p(t, 1, 1, ty).start()
        p(t, 1, 2, tx).start()
        p(t, 0, 3, ty).start()

    def gather_forward(g, buf):
        p = gather_pieces(g, buf)
        p(tx, 0, 0, tx).wait_recv()
        p(tx, 0, 4, ty).start()
        p(ty, 1, 1, ty).wait_recv()
        p(ty, 1, 5, tx).start()

    def gather_near(g, buf):
        p = gather_pieces(g, buf)
        p(tx, 1, 2, tx).wait_recv()
        p(ty, 0, 3, ty).wait_recv()

    def gather_far(g, buf):
        p = gather_pieces(g, buf)
        p(td, 0, 4, ty).wait_recv()
        p(td, 1, 5, tx).wait_recv()

    def gather_drain(g, buf):
        p = gather_pieces(g, buf)
        p(t, 0, 0, tx).wait_send()
        p(t, 1, 1, ty).wait_send()
        p(t, 1, 2, tx).wait_send()
        p(t, 0, 3, ty).wait_send()
        p(tx, 0, 4, ty).wait_send()
        p(ty, 1, 5, tx).wait_send()

    def take_end(u):
        wait_w(u, end)
        send_w(u, end, 2, opp)
        send_w(u, end, 3, partner)

    def pump(u):
        if u + 1 < units:
            take_end(u + 1)
        if u + 4 < units:
            send_w(u + 4, s, 0, opp, own=True)
        wait_w(u, opp)
        send_w(u, opp, 4, partner)
        wait_w(u, oppend)
        send_w(u, oppend, 5, partner)

    def settle(u):
        pltpu.make_async_copy(own_w(u), held_w(u, s), sem_local.at[u]).wait()
        for source in (s, end, opp, oppend):
            wait_w(u, source + flip)

    def project(layer, j, first):
        def tile(r, carry):
            span = pl.ds(pl.multiple_of(r * rows, rows), rows)
            x = xs[layer, j, span, :].astype(f32)
            sq = x * x
            part = sq[:, :128]
            for q in range(1, feats // 128):
                part = part + sq[:, 128 * q : 128 * (q + 1)]
            scaled = (x * gain[layer, pl.ds(j, 1), :]).astype(bf16)
            depth = win.shape[2]
            per = feats // depth
            dots = []
            for m in range(3):
                w = win[3 * layer + m, pl.ds(per * j, per)].reshape(feats, win.shape[3])
                dots.append(jnp.dot(scaled, w, preferred_element_type=f32))
            if first:
                ss[span, :] = part
                for m in range(3):
                    acc[m, span, :] = dots[m]
            else:
                ss[span, :] += part
                for m in range(3):
                    acc[m, span, :] += dots[m]
            return carry
        lax.fori_loop(0, 2, tile, 0)

    def halo_copy(layer):
        count = 2 * rows
        return remote(
            mixed.at[pl.ds(count - 16, 16)], halo.at[layer], h_send.at[layer], h_recv.at[layer], s + 1, t
        )

    def gate(layer):
        width = feats * n_tp
        inv = lax.rsqrt(jnp.sum(ss[...], axis=-1, keepdims=True) / width + eps)
        inner = (acc[1] * inv).astype(bf16)
        value = (acc[2] * inv).astype(bf16)
        mix = (inner.astype(f32) * value.astype(f32)).astype(bf16)
        if layer > 0:
            @pl.when(s < n_sp - 3)
            def _():
                halo_copy(layer - 1).wait_send()
        mixed[...] = mix
        @pl.when(s < n_sp - 3)
        def _():
            halo_copy(layer).start()
        outer = (acc[0] * inv).astype(bf16).astype(f32)
        @pl.when(s == 2)
        def _():
            halo[layer] = jnp.zeros(halo.shape[1:], bf16)
        @pl.when(s > 2)
        def _():
            halo_copy(layer).wait_recv()
        now = mix.astype(f32)
        tail = halo[layer].astype(f32)
        row = lax.broadcasted_iota(jnp.int32, now.shape, 0)
        one = jnp.where(row == 0, tail[15:16], pltpu.roll(now, 1, 0))
        two = pltpu.roll(now, 2, 0)
        two = jnp.where(row == 0, tail[14:15], jnp.where(row == 1, tail[15:16], two))
        conv = taps[layer, 0:1] * two + taps[layer, 1:2] * one + taps[layer, 2:3] * now
        gat[layer, t] = (outer * conv).astype(bf16)

    def back(layer, b):
        span = pl.ds(b * rows, rows)
        total = xs[layer, t, span, :].astype(f32)
        depth = gat.shape[3]
        per = depth // wback.shape[2]
        for j in range(n_tp):
            w = wback[layer, per * j : per * (j + 1)].reshape(depth, feats)
            total = total + jnp.dot(gat[layer, j, span, :], w, preferred_element_type=f32)
        return total.astype(bf16)

    @pl.when(is_mid)
    def _():
        for u in range(min(4, units)):
            send_w(u, s, 0, opp, own=True)
        for u in range(units):
            pltpu.make_async_copy(own_w(u), held_w(u, s), sem_local.at[u]).start()
        @pl.when(outer_mid)
        def _():
            for j in range(n_tp):
                tok_partner(j).start()
        @pl.when(jnp.logical_not(outer_mid))
        def _():
            for j in range(n_tp):
                tok_local(j).start()
        for u in range(units):
            send_w(u, s, 1, partner, own=True)
        take_end(0)
        pump(0)
        first = xs.at[0]
        @pl.when(outer_mid)
        def _():
            for b in range(2):
                place = xs.at[0, t, pl.ds(b * rows, rows)]
                remote(place, place, tok_send.at[b], tok_recv.at[b], partner, t).wait_recv()
            gather_start(0, first)
        pump(1)
        @pl.when(outer_mid)
        def _():
            gather_forward(0, first)
        pump(2)
        @pl.when(outer_mid)
        def _():
            gather_near(0, first)
            gather_far(0, first)
        @pl.when(jnp.logical_not(outer_mid))
        def _():
            for j in range(n_tp):
                tok_local(j).wait()
                tok_partner(j).wait_recv()
        for layer in range(layers):
            for m in range(3):
                settle(4 * layer + m)
            x_g, gate_g = 2 * layer, 2 * layer + 1
            if layer == 0:
                for k, j in enumerate((t, tx, ty, td)):
                    project(layer, j, k == 0)
            else:
                project(layer, t, True)
                gather_near(x_g, xs.at[layer])
                project(layer, tx, False)
                project(layer, ty, False)
                gather_far(x_g, xs.at[layer])
                project(layer, td, False)
            gate(layer)
            gather_start(gate_g, gat.at[layer])
            pump(4 * layer + 3)
            gather_forward(gate_g, gat.at[layer])
            settle(4 * layer + 3)
            gather_near(gate_g, gat.at[layer])
            gather_far(gate_g, gat.at[layer])
            if layer + 1 < layers:
                for b in range(2):
                    xs[layer + 1, t, b * rows : (b + 1) * rows, :] = back(layer, b)
                gather_start(x_g + 2, xs.at[layer + 1])
                pump(4 * layer + 4)
                gather_forward(x_g + 2, xs.at[layer + 1])
                pump(4 * layer + 5)
                pump(4 * layer + 6)
            else:
                for b in range(2):
                    mine = s == (n_sp // 2 - b)
                    res[b] = back(layer, b)
                    @pl.when(mine)
                    def _():
                        out[...] = res[b]
                    @pl.when(jnp.logical_not(mine))
                    def _():
                        result_copy(b).start()
        for u in range(units):
            for kind in range(6):
                remote(own_w(u), held_w(u, s), w_send.at[u, kind], w_recv.at[u, s], partner, t).wait_send()
        for layer in range(layers):
            if layer > 0:
                gather_drain(2 * layer, xs.at[layer])
            gather_drain(2 * layer + 1, gat.at[layer])
        @pl.when(outer_mid)
        def _():
            gather_drain(0, first)
            for j in range(n_tp):
                tok_partner(j).wait_send()
        @pl.when(s < n_sp - 3)
        def _():
            halo_copy(layers - 1).wait_send()
        for b in range(2):
            @pl.when(s != (n_sp // 2 - b))
            def _():
                result_copy(b).wait_send()
        @pl.when(outer_mid)
        def _():
            result_wait()


def fused(tokens, norm_gain, w_outer, w_inner, w_value, w_back, taps):
    n_sp, n_tp = lax.axis_size("sp"), lax.axis_size("tp")
    rows, width = tokens.shape
    layers, depth, chans = w_outer.shape
    back_rows, feats = w_back.shape[1:]
    dma = pltpu.SemaphoreType.DMA
    hbm, vmem = pl.BlockSpec(memory_space=pl.ANY), pl.BlockSpec(memory_space=pltpu.VMEM)
    return pl.pallas_call(
        mixer_kernel,
        out_shape=jax.ShapeDtypeStruct((rows, feats), bf16),
        in_specs=[hbm, vmem, hbm, hbm, hbm, hbm, vmem],
        out_specs=vmem,
        scratch_shapes=[
            pltpu.VMEM((layers, n_tp, 2 * rows, feats), bf16),
            pltpu.VMEM((3 * layers, n_sp, depth, chans), bf16),
            pltpu.VMEM((layers, n_sp, back_rows, feats), bf16),
            pltpu.VMEM((3, 2 * rows, chans), f32),
            pltpu.VMEM((2 * rows, 128), f32),
            pltpu.VMEM((layers, n_tp, 2 * rows, chans), bf16),
            pltpu.VMEM((2 * rows, chans), bf16),
            pltpu.VMEM((layers, 16, chans), bf16),
            pltpu.VMEM((2, rows, feats), bf16),
            pltpu.VMEM((rows, feats), bf16),
            dma((4 * layers,)),
            dma((n_tp,)),
            dma((n_tp,)),
            dma((n_tp,)),
            dma((4 * layers, 6)),
            dma((4 * layers, n_sp)),
            dma((2 * layers, 6)),
            dma((2 * layers, 6)),
            dma((layers,)),
            dma((layers,)),
            dma((2,)),
            dma,
        ],
        compiler_params=pltpu.CompilerParams(
            collective_id=0, has_side_effects=True, vmem_limit_bytes=60 * 1024 * 1024
        ),
        name="mixer",
    )(tokens, norm_gain.reshape(layers, n_tp, feats), w_outer, w_inner, w_value, w_back, taps)


def solution(mesh):
    in_specs = (
        P("sp", None),
        P(),
        P(None, "sp", "tp"),
        P(None, "sp", "tp"),
        P(None, "sp", "tp"),
        P(None, "sp", "tp"),
        P(None, None, "tp"),
    )
    out_specs = P("sp", "tp")
    body = fused if (mesh.shape["sp"], mesh.shape["tp"]) == (8, 4) else per_device
    return jax.shard_map(
        body, mesh=mesh, in_specs=in_specs, out_specs=out_specs, check_vma=False
    )
```

```python
import functools

import jax
import jax.numpy as jnp
from jax import lax
from jax.experimental import pallas as pl
from jax.experimental.pallas import tpu as pltpu
from jax.sharding import PartitionSpec as P

MESH = pl.DeviceIdType.MESH
f32 = jnp.float32
bf16 = jnp.bfloat16

eps = 1e-06


def shifted(block, axis, distance):
    devices = range(lax.axis_size(axis))
    route = [(i - distance, i) for i in devices if i - distance in devices]
    return lax.ppermute(block, axis, route)


def per_device(tokens, norm_gain, w_outer, w_inner, w_value, w_back, taps):
    layers = w_outer.shape[0]
    count = tokens.shape[0]
    feats = w_back.shape[2]
    own = lax.axis_index("tp")
    held = (
        lax.all_gather(w_outer, "sp", axis=1, tiled=True),
        lax.all_gather(w_inner, "sp", axis=1, tiled=True),
        lax.all_gather(w_value, "sp", axis=1, tiled=True),
        lax.all_gather(w_back, "sp", axis=1, tiled=True),
    )
    current = tokens
    resid = lax.dynamic_slice_in_dim(tokens, own * feats, feats, 1)
    for layer in range(layers):
        if layer > 0:
            current = lax.all_gather(resid, "tp", axis=1, tiled=True)
        xf = current.astype(jnp.float32)
        normed = (
            xf * lax.rsqrt(jnp.mean(xf * xf, axis=-1, keepdims=True) + eps) * norm_gain[layer]
        ).astype(jnp.bfloat16)
        outer = jnp.dot(normed, held[0][layer], preferred_element_type=jnp.float32)
        inner = jnp.dot(normed, held[1][layer], preferred_element_type=jnp.float32)
        value = jnp.dot(normed, held[2][layer], preferred_element_type=jnp.float32)
        outer = outer.astype(jnp.bfloat16)
        inner = inner.astype(jnp.bfloat16)
        value = value.astype(jnp.bfloat16)
        mixed = (inner.astype(jnp.float32) * value.astype(jnp.float32)).astype(jnp.bfloat16)
        before = shifted(mixed[count - 2 :], "sp", 1)
        padded = jnp.concatenate([before, mixed], axis=0).astype(jnp.float32)
        conv = (
            taps[layer, 0] * padded[:count]
            + taps[layer, 1] * padded[1 : count + 1]
            + taps[layer, 2] * padded[2:]
        )
        gated = (outer.astype(jnp.float32) * conv).astype(jnp.bfloat16)
        whole = lax.all_gather(gated, "tp", axis=1, tiled=True)
        proj = jnp.dot(whole, held[3][layer], preferred_element_type=jnp.float32)
        resid = (resid.astype(jnp.float32) + proj).astype(jnp.bfloat16)
    return resid


def mixer_kernel(
    tok, gain, w_outer, w_inner, w_value, w_back, taps, out,
    xs, x_last, win, wback, acc, ss, gat, gat_last, mixed, mixed_last, halo, res,
    sem_local, sem_tok_local, tok_send, tok_recv, w_send, w_recv,
    g_send, g_recv, h_send, h_recv, o_send, o_recv,
):
    s, t = lax.axis_index("sp"), lax.axis_index("tp")
    n_sp, n_tp = win.shape[1], x_last.shape[0]
    layers = wback.shape[0]
    rows = tok.shape[0]
    feats = x_last.shape[2]
    units = 4 * layers
    last = layers - 1
    spread = 4 * last
    core = lax.rem(s, 2)
    flip = 1 - 2 * core
    left = s < n_sp // 2
    side = jnp.where(left, 1, -1)
    plane = lax.div(s, 2)
    is_end = jnp.logical_or(plane == 0, plane == n_sp // 2 - 1)
    is_mid = jnp.logical_not(is_end)
    partner = s + flip
    inward = jnp.where(is_end, s + 2 * side, s)
    end = jnp.where(is_mid, s - 2 * side, s)
    opp = jnp.where(is_mid, s + 2 * side, s)
    oppend = jnp.where(is_mid, s + 4 * side, s)
    tx = t + 1 - 2 * lax.rem(t, 2)
    ty = t + 2 - 4 * lax.div(t, 2)
    td = n_tp - 1 - t

    barrier = pltpu.get_barrier_semaphore()
    for k in range(1, n_sp):
        pl.semaphore_signal(barrier, inc=1, device_id=(lax.rem(s + k, n_sp), t), device_id_type=MESH)
    for other in (tx, ty):
        pl.semaphore_signal(barrier, inc=1, device_id=(s, other), device_id_type=MESH)
    pl.semaphore_wait(barrier, n_sp + 1)

    projections = (w_outer, w_inner, w_value)

    def own_w(u):
        layer, m = u // 4, u % 4
        return projections[m].at[layer] if m < 3 else w_back.at[layer]

    def held_w(u, source):
        layer, m = u // 4, u % 4
        return win.at[3 * layer + m, source] if m < 3 else wback.at[layer, source]

    def remote(a, b, ssem, rsem, sp, tp):
        return pltpu.make_async_remote_copy(
            src_ref=a, dst_ref=b, send_sem=ssem, recv_sem=rsem, device_id=(sp, tp), device_id_type=MESH
        )

    def send_w(u, source, kind, target, own=False):
        a = own_w(u) if own else held_w(u, source)
        remote(a, held_w(u, source), w_send.at[u, kind], w_recv.at[u, source], target, t).start()

    def wait_w(u, source):
        remote(held_w(u, source), held_w(u, source), w_send.at[u, 0], w_recv.at[u, source], partner, t).wait_recv()

    def tok_cols(j):
        return tok.at[:, pl.ds(pl.multiple_of(j * feats, feats), feats)]

    def tok_to_end_mid():
        target = lax.div(s, 2) + 2
        place = xs.at[0, t, pl.ds(pl.multiple_of(core * rows, rows), rows)]
        return remote(tok_cols(t), place, tok_send.at[0], tok_recv.at[core], target, t)

    outer_mid = jnp.logical_or(s == 2, s == n_sp - 3)
    my_half = pl.multiple_of(jnp.where(left, 1, 0) * rows, rows)
    partner_half = pl.multiple_of(jnp.where(left, 0, 1) * rows, rows)

    def tok_local(j):
        return pltpu.make_async_copy(tok_cols(j), xs.at[0, j, pl.ds(my_half, rows)], sem_tok_local.at[j])

    def tok_partner(j):
        return remote(tok_cols(j), xs.at[0, j, pl.ds(partner_half, rows)], tok_send.at[j], tok_recv.at[j], partner, t)

    def result_copy(b):
        return remote(res.at[b], x_last.at[t], o_send.at[b], o_recv, 2 * (s - 2) + b, t)


    def gather_pieces(g, buf):
        size = buf.shape[1] // 2
        def piece(block, half, k, target):
            ref = buf.at[block, pl.ds(half * size, size)]
            return remote(ref, ref, g_send.at[g, k], g_recv.at[g, k], s, target)
        return piece

    def gather_start(g, buf):
        p = gather_pieces(g, buf)
        p(t, 0, 0, tx).start()
        p(t, 1, 1, ty).start()
        p(t, 1, 2, tx).start()
        p(t, 0, 3, ty).start()

    def gather_forward(g, buf):
        p = gather_pieces(g, buf)
        p(tx, 0, 0, tx).wait_recv()
        p(tx, 0, 4, ty).start()
        p(ty, 1, 1, ty).wait_recv()
        p(ty, 1, 5, tx).start()

    def gather_near(g, buf):
        p = gather_pieces(g, buf)
        p(tx, 1, 2, tx).wait_recv()
        p(ty, 0, 3, ty).wait_recv()

    def gather_far(g, buf):
        p = gather_pieces(g, buf)
        p(td, 0, 4, ty).wait_recv()
        p(td, 1, 5, tx).wait_recv()

    def gather_drain(g, buf):
        p = gather_pieces(g, buf)
        p(t, 0, 0, tx).wait_send()
        p(t, 1, 1, ty).wait_send()
        p(t, 1, 2, tx).wait_send()
        p(t, 0, 3, ty).wait_send()
        p(tx, 0, 4, ty).wait_send()
        p(ty, 1, 5, tx).wait_send()

    def take_end(u):
        wait_w(u, end)
        send_w(u, end, 2, opp)
        send_w(u, end, 3, partner)

    def pump(u):
        if u + 1 < units:
            take_end(u + 1)
        if u + 4 < units:
            send_w(u + 4, s, 0, opp, own=True)
        wait_w(u, opp)
        if u >= spread:
            send_w(u, opp, 7, end)
        send_w(u, opp, 4, partner)
        wait_w(u, oppend)
        if u >= spread:
            send_w(u, oppend, 8, end)
        send_w(u, oppend, 5, partner)

    def end_feed(u):
        for k in (1, 2, 3):
            source = s + 2 * k * side
            wait_w(u, source)
            send_w(u, source, 2 + k, partner)

    def feed(u):
        @pl.when(is_mid)
        def _():
            pump(u)
        @pl.when(is_end)
        def _():
            end_feed(u)

    def settle(u):
        pltpu.make_async_copy(own_w(u), held_w(u, s), sem_local.at[u]).wait()
        for source in range(0, n_sp, 2):
            wait_w(u, source + 1 - core)

    def project(layer, x_ref, j, first):
        def tile(r, carry):
            span = pl.ds(pl.multiple_of(r * rows, rows), rows)
            x = x_ref[j, span, :].astype(f32)
            sq = x * x
            part = sq[:, :128]
            for q in range(1, feats // 128):
                part = part + sq[:, 128 * q : 128 * (q + 1)]
            scaled = (x * gain[layer : layer + 1, pl.ds(pl.multiple_of(j * feats, feats), feats)]).astype(bf16)
            depth = win.shape[2]
            per = feats // depth
            dots = []
            for m in range(3):
                w = win[3 * layer + m, pl.ds(per * j, per)].reshape(feats, win.shape[3])
                dots.append(jnp.dot(scaled, w, preferred_element_type=f32))
            if first:
                ss[span, :] = part
                for m in range(3):
                    acc[m, span, :] = dots[m]
            else:
                ss[span, :] += part
                for m in range(3):
                    acc[m, span, :] += dots[m]
            return carry
        lax.fori_loop(0, x_ref.shape[1] // rows, tile, 0)

    def halo_copy(layer, mix_ref):
        count = mix_ref.shape[0]
        return remote(
            mix_ref.at[pl.ds(count - 16, 16)], halo.at[layer], h_send.at[layer], h_recv.at[layer], s + 1, t
        )

    def gate(layer, mix_ref, gat_ref, begin, final):
        width = feats * n_tp
        span = pl.ds(0, mix_ref.shape[0])
        inv = lax.rsqrt(jnp.sum(ss[span, :], axis=-1, keepdims=True) / width + eps)
        inner = (acc[1, span, :] * inv).astype(bf16)
        value = (acc[2, span, :] * inv).astype(bf16)
        mix = (inner.astype(f32) * value.astype(f32)).astype(bf16)
        mix_ref[...] = mix
        @pl.when(s < final)
        def _():
            halo_copy(layer, mix_ref).start()
        outer = (acc[0, span, :] * inv).astype(bf16).astype(f32)
        @pl.when(s == begin)
        def _():
            halo[layer] = jnp.zeros(halo.shape[1:], bf16)
        @pl.when(s > begin)
        def _():
            halo_copy(layer, mix_ref).wait_recv()
        now = mix.astype(f32)
        tail = halo[layer].astype(f32)
        row = lax.broadcasted_iota(jnp.int32, now.shape, 0)
        one = jnp.where(row == 0, tail[15:16], pltpu.roll(now, 1, 0))
        two = pltpu.roll(now, 2, 0)
        two = jnp.where(row == 0, tail[14:15], jnp.where(row == 1, tail[15:16], two))
        conv = taps[layer, 0:1] * two + taps[layer, 1:2] * one + taps[layer, 2:3] * now
        gat_ref[t] = (outer * conv).astype(bf16)

    def back(layer, x_ref, gat_ref, b):
        span = pl.ds(b * rows, rows)
        total = x_ref[t, span, :].astype(f32)
        depth = gat_ref.shape[2]
        per = depth // wback.shape[2]
        for j in range(n_tp):
            w = wback[layer, per * j : per * (j + 1)].reshape(depth, feats)
            total = total + jnp.dot(gat_ref[j, span, :], w, preferred_element_type=f32)
        return total.astype(bf16)

    def mine(b):
        return s == n_sp // 2 - b

    for u in range(units):
        @pl.when(jnp.logical_or(is_mid, u >= spread))
        def _():
            pltpu.make_async_copy(own_w(u), held_w(u, s), sem_local.at[u]).start()

    @pl.when(is_end)
    def _():
        for u in range(units):
            send_w(u, s, 0, inward, own=True)
            if u == 0:
                tok_to_end_mid().start()
        for u in range(spread, units):
            send_w(u, s, 1, partner, own=True)

    @pl.when(is_mid)
    def _():
        for u in range(min(4, units)):
            send_w(u, s, 0, opp, own=True)
        for u in range(spread, units):
            send_w(u, s, 6, end, own=True)
        @pl.when(outer_mid)
        def _():
            for j in range(n_tp):
                tok_partner(j).start()
        @pl.when(jnp.logical_not(outer_mid))
        def _():
            for j in range(n_tp):
                tok_local(j).start()
        for u in range(units):
            send_w(u, s, 1, partner, own=True)
        take_end(0)
        pump(0)
        first = xs.at[0]
        @pl.when(outer_mid)
        def _():
            for b in range(2):
                place = xs.at[0, t, pl.ds(b * rows, rows)]
                remote(place, place, tok_send.at[b], tok_recv.at[b], partner, t).wait_recv()
            gather_start(0, first)
        pump(1)
        @pl.when(outer_mid)
        def _():
            gather_forward(0, first)
        pump(2)
        @pl.when(outer_mid)
        def _():
            gather_near(0, first)
            gather_far(0, first)
        @pl.when(jnp.logical_not(outer_mid))
        def _():
            for j in range(n_tp):
                tok_local(j).wait()
                tok_partner(j).wait_recv()
        for layer in range(last):
            x_ref, gat_ref = xs.at[layer], gat.at[layer]
            if layer > 0:
                for m in range(3):
                    pump(4 * layer + m)
                gather_forward(2 * layer, x_ref)
                gather_near(2 * layer, x_ref)
                gather_far(2 * layer, x_ref)
            for m in range(3):
                settle(4 * layer + m)
            for k, j in enumerate((t, tx, ty, td)):
                project(layer, x_ref, j, k == 0)
            gate(layer, mixed.at[layer], gat_ref, 2, n_sp - 3)
            gather_start(2 * layer + 1, gat_ref)
            pump(4 * layer + 3)
            gather_forward(2 * layer + 1, gat_ref)
            settle(4 * layer + 3)
            gather_near(2 * layer + 1, gat_ref)
            gather_far(2 * layer + 1, gat_ref)
            for b in range(2):
                if layer + 1 < last:
                    xs[layer + 1, t, b * rows : (b + 1) * rows, :] = back(layer, x_ref, gat_ref, b)
                else:
                    res[b] = back(layer, x_ref, gat_ref, b)
                    @pl.when(mine(b))
                    def _():
                        x_last[t] = res[b]
                    @pl.when(jnp.logical_not(mine(b)))
                    def _():
                        result_copy(b).start()
            if layer + 1 < last:
                gather_start(2 * layer + 2, xs.at[layer + 1])

    @pl.when(jnp.logical_not(jnp.logical_or(mine(0), mine(1))))
    def _():
        remote(res.at[0], x_last.at[t], o_send.at[0], o_recv, partner, t).wait_recv()
    gather_start(2 * last, x_last)
    feed(spread)
    gather_forward(2 * last, x_last)
    feed(spread + 1)
    feed(spread + 2)
    for m in range(3):
        settle(spread + m)
    project(last, x_last, t, True)
    gather_near(2 * last, x_last)
    project(last, x_last, tx, False)
    project(last, x_last, ty, False)
    gather_far(2 * last, x_last)
    project(last, x_last, td, False)
    gate(last, mixed_last, gat_last, 0, n_sp - 1)
    gather_start(2 * last + 1, gat_last)
    feed(spread + 3)
    gather_forward(2 * last + 1, gat_last)
    settle(spread + 3)
    gather_near(2 * last + 1, gat_last)
    gather_far(2 * last + 1, gat_last)
    out[...] = back(last, x_last, gat_last, 0)

    def sent_w(u, kind):
        remote(own_w(u), held_w(u, s), w_send.at[u, kind], w_recv.at[u, s], partner, t).wait_send()

    @pl.when(is_end)
    def _():
        for u in range(units):
            for kind in (0, 1, 3, 4, 5) if u >= spread else (0,):
                sent_w(u, kind)
        tok_to_end_mid().wait_send()

    @pl.when(is_mid)
    def _():
        for u in range(units):
            for kind in range(9 if u >= spread else 6):
                sent_w(u, kind)
        for layer in range(last):
            if layer > 0:
                gather_drain(2 * layer, xs.at[layer])
            gather_drain(2 * layer + 1, gat.at[layer])
            @pl.when(s < n_sp - 3)
            def _():
                halo_copy(layer, mixed.at[layer]).wait_send()
        @pl.when(outer_mid)
        def _():
            gather_drain(0, xs.at[0])
            for j in range(n_tp):
                tok_partner(j).wait_send()
        for b in range(2):
            @pl.when(jnp.logical_not(mine(b)))
            def _():
                result_copy(b).wait_send()

    gather_drain(2 * last, x_last)
    gather_drain(2 * last + 1, gat_last)
    @pl.when(s < n_sp - 1)
    def _():
        halo_copy(last, mixed_last).wait_send()


def fused(tokens, norm_gain, w_outer, w_inner, w_value, w_back, taps):
    n_sp, n_tp = lax.axis_size("sp"), lax.axis_size("tp")
    rows, width = tokens.shape
    layers, depth, chans = w_outer.shape
    back_rows, feats = w_back.shape[1:]
    dma = pltpu.SemaphoreType.DMA
    hbm, vmem = pl.BlockSpec(memory_space=pl.ANY), pl.BlockSpec(memory_space=pltpu.VMEM)
    return pl.pallas_call(
        mixer_kernel,
        out_shape=jax.ShapeDtypeStruct((rows, feats), bf16),
        in_specs=[hbm, vmem, hbm, hbm, hbm, hbm, vmem],
        out_specs=vmem,
        scratch_shapes=[
            pltpu.VMEM((layers - 1, n_tp, 2 * rows, feats), bf16),
            pltpu.VMEM((n_tp, rows, feats), bf16),
            pltpu.VMEM((3 * layers, n_sp, depth, chans), bf16),
            pltpu.VMEM((layers, n_sp, back_rows, feats), bf16),
            pltpu.VMEM((3, 2 * rows, chans), f32),
            pltpu.VMEM((2 * rows, 128), f32),
            pltpu.VMEM((layers - 1, n_tp, 2 * rows, chans), bf16),
            pltpu.VMEM((n_tp, rows, chans), bf16),
            pltpu.VMEM((layers - 1, 2 * rows, chans), bf16),
            pltpu.VMEM((rows, chans), bf16),
            pltpu.VMEM((layers, 16, chans), bf16),
            pltpu.VMEM((2, rows, feats), bf16),
            dma((4 * layers,)),
            dma((n_tp,)),
            dma((n_tp,)),
            dma((n_tp,)),
            dma((4 * layers, 9)),
            dma((4 * layers, n_sp)),
            dma((2 * layers, 6)),
            dma((2 * layers, 6)),
            dma((layers,)),
            dma((layers,)),
            dma((2,)),
            dma,
        ],
        compiler_params=pltpu.CompilerParams(
            collective_id=0, has_side_effects=True, vmem_limit_bytes=60 * 1024 * 1024
        ),
        name="mixer",
    )(tokens, norm_gain, w_outer, w_inner, w_value, w_back, taps)


def solution(mesh):
    in_specs = (
        P("sp", None),
        P(),
        P(None, "sp", "tp"),
        P(None, "sp", "tp"),
        P(None, "sp", "tp"),
        P(None, "sp", "tp"),
        P(None, None, "tp"),
    )
    out_specs = P("sp", "tp")
    body = fused if (mesh.shape["sp"], mesh.shape["tp"]) == (8, 4) else per_device
    return jax.shard_map(
        body, mesh=mesh, in_specs=in_specs, out_specs=out_specs, check_vma=False
    )
```

```python
import functools

import jax
import jax.numpy as jnp
from jax import lax
from jax.experimental import pallas as pl
from jax.experimental.pallas import tpu as pltpu
from jax.sharding import PartitionSpec as P

MESH = pl.DeviceIdType.MESH
f32 = jnp.float32
bf16 = jnp.bfloat16

eps = 1e-06


def shifted(block, axis, distance):
    devices = range(lax.axis_size(axis))
    route = [(i - distance, i) for i in devices if i - distance in devices]
    return lax.ppermute(block, axis, route)


def per_device(tokens, norm_gain, w_outer, w_inner, w_value, w_back, taps):
    layers = w_outer.shape[0]
    count = tokens.shape[0]
    feats = w_back.shape[2]
    own = lax.axis_index("tp")
    held = (
        lax.all_gather(w_outer, "sp", axis=1, tiled=True),
        lax.all_gather(w_inner, "sp", axis=1, tiled=True),
        lax.all_gather(w_value, "sp", axis=1, tiled=True),
        lax.all_gather(w_back, "sp", axis=1, tiled=True),
    )
    current = tokens
    resid = lax.dynamic_slice_in_dim(tokens, own * feats, feats, 1)
    for layer in range(layers):
        if layer > 0:
            current = lax.all_gather(resid, "tp", axis=1, tiled=True)
        xf = current.astype(jnp.float32)
        normed = (
            xf * lax.rsqrt(jnp.mean(xf * xf, axis=-1, keepdims=True) + eps) * norm_gain[layer]
        ).astype(jnp.bfloat16)
        outer = jnp.dot(normed, held[0][layer], preferred_element_type=jnp.float32)
        inner = jnp.dot(normed, held[1][layer], preferred_element_type=jnp.float32)
        value = jnp.dot(normed, held[2][layer], preferred_element_type=jnp.float32)
        outer = outer.astype(jnp.bfloat16)
        inner = inner.astype(jnp.bfloat16)
        value = value.astype(jnp.bfloat16)
        mixed = (inner.astype(jnp.float32) * value.astype(jnp.float32)).astype(jnp.bfloat16)
        before = shifted(mixed[count - 2 :], "sp", 1)
        padded = jnp.concatenate([before, mixed], axis=0).astype(jnp.float32)
        conv = (
            taps[layer, 0] * padded[:count]
            + taps[layer, 1] * padded[1 : count + 1]
            + taps[layer, 2] * padded[2:]
        )
        gated = (outer.astype(jnp.float32) * conv).astype(jnp.bfloat16)
        whole = lax.all_gather(gated, "tp", axis=1, tiled=True)
        proj = jnp.dot(whole, held[3][layer], preferred_element_type=jnp.float32)
        resid = (resid.astype(jnp.float32) + proj).astype(jnp.bfloat16)
    return resid


def mixer_kernel(
    tok, gain, w_outer, w_inner, w_value, w_back, taps, out,
    xs, win, wback, acc, ss, gat, mixed, halo, res, landed,
    sem_local, sem_tok_local, tok_send, tok_recv, w_send, w_recv,
    g_send, g_recv, h_send, h_recv, o_send, o_recv,
):
    s, t = lax.axis_index("sp"), lax.axis_index("tp")
    n_sp, n_tp = win.shape[1], xs.shape[1]
    layers = wback.shape[0]
    rows = tok.shape[0]
    feats = xs.shape[3]
    units = 4 * layers
    core = lax.rem(s, 2)
    flip = 1 - 2 * core
    left = s < n_sp // 2
    side = jnp.where(left, 1, -1)
    plane = lax.div(s, 2)
    is_end = jnp.logical_or(plane == 0, plane == n_sp // 2 - 1)
    is_mid = jnp.logical_not(is_end)
    partner = s + flip
    inward = jnp.where(is_end, s + 2 * side, s)
    end = jnp.where(is_mid, s - 2 * side, s)
    opp = jnp.where(is_mid, s + 2 * side, s)
    oppend = jnp.where(is_mid, s + 4 * side, s)
    tx = t + 1 - 2 * lax.rem(t, 2)
    ty = t + 2 - 4 * lax.div(t, 2)
    td = n_tp - 1 - t

    barrier = pltpu.get_barrier_semaphore()
    for k in range(1, n_sp):
        pl.semaphore_signal(barrier, inc=1, device_id=(lax.rem(s + k, n_sp), t), device_id_type=MESH)
    for other in (tx, ty):
        pl.semaphore_signal(barrier, inc=1, device_id=(s, other), device_id_type=MESH)
    pl.semaphore_wait(barrier, n_sp + 1)

    projections = (w_outer, w_inner, w_value)

    def own_w(u):
        layer, m = u // 4, u % 4
        return projections[m].at[layer] if m < 3 else w_back.at[layer]

    def held_w(u, source):
        layer, m = u // 4, u % 4
        return win.at[3 * layer + m, source] if m < 3 else wback.at[layer, source]

    def remote(a, b, ssem, rsem, sp, tp):
        return pltpu.make_async_remote_copy(
            src_ref=a, dst_ref=b, send_sem=ssem, recv_sem=rsem, device_id=(sp, tp), device_id_type=MESH
        )

    def send_w(u, source, kind, target, own=False):
        a = own_w(u) if own else held_w(u, source)
        remote(a, held_w(u, source), w_send.at[u, kind], w_recv.at[u, source], target, t).start()

    def wait_w(u, source):
        remote(held_w(u, source), held_w(u, source), w_send.at[u, 0], w_recv.at[u, source], partner, t).wait_recv()

    def tok_cols(j):
        return tok.at[:, pl.ds(pl.multiple_of(j * feats, feats), feats)]

    def tok_to_end_mid():
        target = lax.div(s, 2) + 2
        place = xs.at[0, t, pl.ds(pl.multiple_of(core * rows, rows), rows)]
        return remote(tok_cols(t), place, tok_send.at[0], tok_recv.at[core], target, t)

    outer_mid = jnp.logical_or(s == 2, s == n_sp - 3)
    my_half = pl.multiple_of(jnp.where(left, 1, 0) * rows, rows)
    partner_half = pl.multiple_of(jnp.where(left, 0, 1) * rows, rows)

    def tok_local(j):
        return pltpu.make_async_copy(tok_cols(j), xs.at[0, j, pl.ds(my_half, rows)], sem_tok_local.at[j])

    def tok_partner(j):
        return remote(tok_cols(j), xs.at[0, j, pl.ds(partner_half, rows)], tok_send.at[j], tok_recv.at[j], partner, t)

    def result_copy(b):
        return remote(res.at[b], landed, o_send.at[b], o_recv, 2 * (s - 2) + b, t)

    def result_wait():
        remote(landed, landed, o_send.at[0], o_recv, partner, t).wait_recv()
        out[...] = landed[...]

    @pl.when(is_end)
    def _():
        sends = []
        for u in range(units):
            send_w(u, s, 0, inward, own=True)
            if u == 0:
                tok_to_end_mid().start()
        for u in range(units):
            remote(own_w(u), held_w(u, s), w_send.at[u, 0], w_recv.at[u, s], inward, t).wait_send()
        tok_to_end_mid().wait_send()
        result_wait()

    def gather_pieces(g, buf):
        size = buf.shape[1] // 2
        def piece(block, half, k, target):
            ref = buf.at[block, pl.ds(half * size, size)]
            return remote(ref, ref, g_send.at[g, k], g_recv.at[g, k], s, target)
        return piece

    def gather_start(g, buf):
        p = gather_pieces(g, buf)
        p(t, 0, 0, tx).start()
        p(t, 1, 1, ty).start()
        p(t, 1, 2, tx).start()
        p(t, 0, 3, ty).start()

    def gather_forward(g, buf):
        p = gather_pieces(g, buf)
        p(tx, 0, 0, tx).wait_recv()
        p(tx, 0, 4, ty).start()
        p(ty, 1, 1, ty).wait_recv()
        p(ty, 1, 5, tx).start()

    def gather_near(g, buf):
        p = gather_pieces(g, buf)
        p(tx, 1, 2, tx).wait_recv()
        p(ty, 0, 3, ty).wait_recv()

    def gather_far(g, buf):
        p = gather_pieces(g, buf)
        p(td, 0, 4, ty).wait_recv()
        p(td, 1, 5, tx).wait_recv()

    def gather_drain(g, buf):
        p = gather_pieces(g, buf)
        p(t, 0, 0, tx).wait_send()
        p(t, 1, 1, ty).wait_send()
        p(t, 1, 2, tx).wait_send()
        p(t, 0, 3, ty).wait_send()
        p(tx, 0, 4, ty).wait_send()
        p(ty, 1, 5, tx).wait_send()

    def take_end(u):
        wait_w(u, end)
        send_w(u, end, 2, opp)
        send_w(u, end, 3, partner)

    def pump(u):
        if u + 1 < units:
            take_end(u + 1)
        if u + 4 < units:
            send_w(u + 4, s, 0, opp, own=True)
        wait_w(u, opp)
        send_w(u, opp, 4, partner)
        wait_w(u, oppend)
        send_w(u, oppend, 5, partner)

    def settle(u):
        pltpu.make_async_copy(own_w(u), held_w(u, s), sem_local.at[u]).wait()
        for source in (s, end, opp, oppend):
            wait_w(u, source + flip)

    def project(layer, j, first):
        def tile(r, carry):
            span = pl.ds(pl.multiple_of(r * rows, rows), rows)
            x = xs[layer, j, span, :].astype(f32)
            sq = x * x
            part = sq[:, :128]
            for q in range(1, feats // 128):
                part = part + sq[:, 128 * q : 128 * (q + 1)]
            scaled = (x * gain[layer : layer + 1, pl.ds(pl.multiple_of(j * feats, feats), feats)]).astype(bf16)
            depth = win.shape[2]
            per = feats // depth
            dots = []
            for m in range(3):
                w = win[3 * layer + m, pl.ds(per * j, per)].reshape(feats, win.shape[3])
                dots.append(jnp.dot(scaled, w, preferred_element_type=f32))
            if first:
                ss[span, :] = part
                for m in range(3):
                    acc[m, span, :] = dots[m]
            else:
                ss[span, :] += part
                for m in range(3):
                    acc[m, span, :] += dots[m]
            return carry
        lax.fori_loop(0, 2, tile, 0)

    def halo_copy(layer):
        count = 2 * rows
        return remote(
            mixed.at[pl.ds(count - 16, 16)], halo.at[layer], h_send.at[layer], h_recv.at[layer], s + 1, t
        )

    def gate(layer):
        width = feats * n_tp
        inv = lax.rsqrt(jnp.sum(ss[...], axis=-1, keepdims=True) / width + eps)
        inner = (acc[1] * inv).astype(bf16)
        value = (acc[2] * inv).astype(bf16)
        mix = (inner.astype(f32) * value.astype(f32)).astype(bf16)
        if layer > 0:
            @pl.when(s < n_sp - 3)
            def _():
                halo_copy(layer - 1).wait_send()
        mixed[...] = mix
        @pl.when(s < n_sp - 3)
        def _():
            halo_copy(layer).start()
        outer = (acc[0] * inv).astype(bf16).astype(f32)
        @pl.when(s == 2)
        def _():
            halo[layer] = jnp.zeros(halo.shape[1:], bf16)
        @pl.when(s > 2)
        def _():
            halo_copy(layer).wait_recv()
        now = mix.astype(f32)
        tail = halo[layer].astype(f32)
        row = lax.broadcasted_iota(jnp.int32, now.shape, 0)
        one = jnp.where(row == 0, tail[15:16], pltpu.roll(now, 1, 0))
        two = pltpu.roll(now, 2, 0)
        two = jnp.where(row == 0, tail[14:15], jnp.where(row == 1, tail[15:16], two))
        conv = taps[0, layer : layer + 1] * two + taps[1, layer : layer + 1] * one + taps[2, layer : layer + 1] * now
        gat[layer, t] = (outer * conv).astype(bf16)

    def back(layer, b):
        span = pl.ds(b * rows, rows)
        total = xs[layer, t, span, :].astype(f32)
        depth = gat.shape[3]
        per = depth // wback.shape[2]
        for j in range(n_tp):
            w = wback[layer, per * j : per * (j + 1)].reshape(depth, feats)
            total = total + jnp.dot(gat[layer, j, span, :], w, preferred_element_type=f32)
        return total.astype(bf16)

    @pl.when(is_mid)
    def _():
        for u in range(min(4, units)):
            send_w(u, s, 0, opp, own=True)
        for u in range(units):
            pltpu.make_async_copy(own_w(u), held_w(u, s), sem_local.at[u]).start()
        @pl.when(outer_mid)
        def _():
            for j in range(n_tp):
                tok_partner(j).start()
        @pl.when(jnp.logical_not(outer_mid))
        def _():
            for j in range(n_tp):
                tok_local(j).start()
        for u in range(units):
            send_w(u, s, 1, partner, own=True)
        take_end(0)
        first = xs.at[0]
        @pl.when(outer_mid)
        def _():
            for b in range(2):
                place = xs.at[0, t, pl.ds(b * rows, rows)]
                remote(place, place, tok_send.at[b], tok_recv.at[b], partner, t).wait_recv()
            gather_start(0, first)
        pump(0)
        @pl.when(outer_mid)
        def _():
            gather_forward(0, first)
        pump(1)
        pump(2)
        @pl.when(outer_mid)
        def _():
            gather_near(0, first)
            gather_far(0, first)
        @pl.when(jnp.logical_not(outer_mid))
        def _():
            for j in range(n_tp):
                tok_local(j).wait()
                tok_partner(j).wait_recv()
        for layer in range(layers):
            for m in range(3):
                settle(4 * layer + m)
            x_g, gate_g = 2 * layer, 2 * layer + 1
            if layer == 0:
                for k, j in enumerate((t, tx, ty, td)):
                    project(layer, j, k == 0)
            else:
                project(layer, t, True)
                gather_near(x_g, xs.at[layer])
                project(layer, tx, False)
                project(layer, ty, False)
                gather_far(x_g, xs.at[layer])
                project(layer, td, False)
            gate(layer)
            g = gather_pieces(gate_g, gat.at[layer])
            g(t, 0, 0, tx).start()
            g(t, 0, 3, ty).start()
            g(t, 1, 1, ty).start()
            g(t, 1, 2, tx).start()
            pump(4 * layer + 3)
            g(tx, 0, 0, tx).wait_recv()
            g(tx, 0, 4, ty).start()
            g(ty, 1, 1, ty).wait_recv()
            g(ty, 1, 5, tx).start()
            settle(4 * layer + 3)

            def take_gated(b):
                if b == 0:
                    g(ty, 0, 3, ty).wait_recv()
                    g(td, 0, 4, ty).wait_recv()
                else:
                    g(tx, 1, 2, tx).wait_recv()
                    g(td, 1, 5, tx).wait_recv()

            if layer + 1 < layers:
                for b in range(2):
                    take_gated(b)
                    xs[layer + 1, t, b * rows : (b + 1) * rows, :] = back(layer, b)
                gather_start(x_g + 2, xs.at[layer + 1])
                pump(4 * layer + 4)
                gather_forward(x_g + 2, xs.at[layer + 1])
                pump(4 * layer + 5)
                pump(4 * layer + 6)
            else:
                for b in range(2):
                    mine = s == (n_sp // 2 - b)
                    take_gated(b)
                    res[b] = back(layer, b)
                    @pl.when(mine)
                    def _():
                        out[...] = res[b]
                    @pl.when(jnp.logical_not(mine))
                    def _():
                        result_copy(b).start()
        for u in range(units):
            for kind in range(6):
                remote(own_w(u), held_w(u, s), w_send.at[u, kind], w_recv.at[u, s], partner, t).wait_send()
        for layer in range(layers):
            if layer > 0:
                gather_drain(2 * layer, xs.at[layer])
            gather_drain(2 * layer + 1, gat.at[layer])
        @pl.when(outer_mid)
        def _():
            gather_drain(0, first)
            for j in range(n_tp):
                tok_partner(j).wait_send()
        @pl.when(s < n_sp - 3)
        def _():
            halo_copy(layers - 1).wait_send()
        for b in range(2):
            @pl.when(s != (n_sp // 2 - b))
            def _():
                result_copy(b).wait_send()
        @pl.when(outer_mid)
        def _():
            result_wait()


def fused(tokens, norm_gain, w_outer, w_inner, w_value, w_back, taps):
    n_sp, n_tp = lax.axis_size("sp"), lax.axis_size("tp")
    rows, width = tokens.shape
    layers, depth, chans = w_outer.shape
    back_rows, feats = w_back.shape[1:]
    dma = pltpu.SemaphoreType.DMA
    hbm, vmem = pl.BlockSpec(memory_space=pl.ANY), pl.BlockSpec(memory_space=pltpu.VMEM)
    return pl.pallas_call(
        mixer_kernel,
        out_shape=jax.ShapeDtypeStruct((rows, feats), bf16),
        in_specs=[hbm, vmem, hbm, hbm, hbm, hbm, vmem],
        out_specs=vmem,
        scratch_shapes=[
            pltpu.VMEM((layers, n_tp, 2 * rows, feats), bf16),
            pltpu.VMEM((3 * layers, n_sp, depth, chans), bf16),
            pltpu.VMEM((layers, n_sp, back_rows, feats), bf16),
            pltpu.VMEM((3, 2 * rows, chans), f32),
            pltpu.VMEM((2 * rows, 128), f32),
            pltpu.VMEM((layers, n_tp, 2 * rows, chans), bf16),
            pltpu.VMEM((2 * rows, chans), bf16),
            pltpu.VMEM((layers, 16, chans), bf16),
            pltpu.VMEM((2, rows, feats), bf16),
            pltpu.VMEM((rows, feats), bf16),
            dma((4 * layers,)),
            dma((n_tp,)),
            dma((n_tp,)),
            dma((n_tp,)),
            dma((4 * layers, 6)),
            dma((4 * layers, n_sp)),
            dma((2 * layers, 6)),
            dma((2 * layers, 6)),
            dma((layers,)),
            dma((layers,)),
            dma((2,)),
            dma,
        ],
        compiler_params=pltpu.CompilerParams(
            collective_id=0, has_side_effects=True, vmem_limit_bytes=60 * 1024 * 1024
        ),
        name="mixer",
    )(tokens, norm_gain, w_outer, w_inner, w_value, w_back, taps.transpose(1, 0, 2))


def solution(mesh):
    in_specs = (
        P("sp", None),
        P(),
        P(None, "sp", "tp"),
        P(None, "sp", "tp"),
        P(None, "sp", "tp"),
        P(None, "sp", "tp"),
        P(None, None, "tp"),
    )
    out_specs = P("sp", "tp")
    body = fused if (mesh.shape["sp"], mesh.shape["tp"]) == (8, 4) else per_device
    return jax.shard_map(
        body, mesh=mesh, in_specs=in_specs, out_specs=out_specs, check_vma=False
    )
```
